32 devices in a mesh: fs: 8 (over z, x), tp: 4 (over y, core).
Axes of the slice: x: 2, y: 2, z: 4, core: 2. Of those that a mesh axis runs over, the one named last changes fastest.
Arguments:
- tokens: bfloat16 [8192, 2048], P(('fs', 'tp')), may hold values from -6 to 6
- gate_pre: bfloat16 [8192, 5632], P('fs', 'tp'), may hold values from -6 to 6
- value_pre: bfloat16 [8192, 5632], P('fs', 'tp'), may hold values from -6 to 6
- up_gate_w: bfloat16 [2048, 5632], P('fs', 'tp'), may hold values from -0.078125 to 0.078125
- up_value_w: bfloat16 [2048, 5632], P('fs', 'tp'), may hold values from -0.078125 to 0.078125
- conv_weight: float32 [3, 5632], P(None, 'tp'), may hold values from -3 to 3
- conv_bias: float32 [5632], P('tp'), may hold values from -3 to 3
- hidden_grad: bfloat16 [8192, 5632], P('fs', 'tp'), may hold values from -6 to 6
Outputs:
- input_grad: bfloat16 [8192, 2048], P(('fs', 'tp'))
- up_gate_grad: float32 [2048, 5632], P('fs', 'tp')
- up_value_grad: float32 [2048, 5632], P('fs', 'tp')
- conv_weight_grad: float32 [3, 5632], P(None, 'tp')
- conv_bias_grad: float32 [5632], P('tp')
The draws below stay inside these ranges and needn't reach their ends.
All inputs are finite; a program needn't handle non-finite values.
Results may differ from the reference program's by a relative error of at most 0.013.
Values may be sent and summed in bfloat16 or wider, within the bound.
A program may use at most 128 MiB of HBM per device.

```python
import jax
import jax.numpy as jnp
from jax import lax

D = 2048
FF = 5632
ROWS = 1024
TOKENS = 8192
N_FS = 8
N_TP = 4


def with_spikes(result, rng, source, target, shards_of, factor):
    owner, partner = [(jnp.arange(result.shape[dim]) // (result.shape[dim] // shards_of)).reshape([-1 if axis == dim else 1 for axis in range(result.ndim)]) for dim in (source, target)]
    chosen = jax.random.permutation(rng, shards_of)[partner]
    strong = (owner == chosen) | (owner == (partner + shards_of // 2) % shards_of)
    return jnp.where(strong, factor * result, result)


def block_scale(stream_key, shape, cuts, low, largest):
    def one(dim, blocks):
        draws = jax.random.uniform(jax.random.fold_in(jax.random.fold_in(stream_key, 6), dim), (blocks,), jnp.float32, low / len(cuts), largest / len(cuts))
        return jnp.repeat(jnp.exp(draws), shape[dim] // blocks).reshape((-1,) + (1,) * (len(shape) - dim - 1))

    loudness = one(*cuts[0])
    for cut in cuts[1:]:
        loudness = loudness * one(*cut)
    return loudness


def scatter_about(stream_key, dims, spread, limit, shards=(), kind=jnp.bfloat16):
    entries = spread * jax.random.normal(stream_key, dims, jnp.float32)
    if shards:
        entries = entries * block_scale(stream_key, dims, shards, -0.22, 0.18)
    return jnp.clip(entries, -limit, limit).astype(kind)


def heavy_noise(stream_key, dims, deviation, reach, shards, heavy, dtype=jnp.bfloat16):
    result = deviation * jax.random.normal(stream_key, dims, jnp.float32)
    if shards:
        result = result * block_scale(stream_key, dims, shards, -0.22, 0.18)
    return jnp.clip(with_spikes(result, jax.random.fold_in(stream_key, 3), *heavy), -reach, reach).astype(dtype)


def setup_inputs(seed: int = 0) -> dict:
    splits = jax.random.split(jax.random.key(seed), 9)
    tokens = scatter_about(splits[0], (TOKENS, D), 1.0, 6.0, ((0, 32),))
    gate_pre = scatter_about(splits[1], (TOKENS, FF), 1.0, 6.0, ((0, 8), (1, 4)))
    value_pre = scatter_about(splits[2], (TOKENS, FF), 1.0, 6.0, ((0, 8), (1, 4)))
    up_gate_w = scatter_about(splits[3], (D, FF), FF ** -0.5, 0.078125, ((0, 8), (1, 4)))
    up_value_w = scatter_about(splits[4], (D, FF), FF ** -0.5, 0.078125, ((0, 8), (1, 4)))
    conv_weight = scatter_about(splits[5], (3, FF), 0.6, 3.0, ((1, 4),), jnp.float32)
    conv_bias = scatter_about(splits[6], (FF,), 0.5, 3.0, ((0, 4),), jnp.float32)
    hidden_grad = heavy_noise(splits[7], (TOKENS, FF), 1.0, 6.0, ((0, 8), (1, 4)), (0, 1, 8, 2.0))
    return dict(tokens=tokens, gate_pre=gate_pre, value_pre=value_pre, up_gate_w=up_gate_w, up_value_w=up_value_w, conv_weight=conv_weight, conv_bias=conv_bias, hidden_grad=hidden_grad)


def conv_forward(pre_gate, conv_weight, conv_bias):
    length = pre_gate.shape[0]
    padded = jnp.pad(pre_gate, ((2, 0), (0, 0)))
    return conv_bias + conv_weight[0] * padded[:length] + conv_weight[1] * padded[1:length + 1] + conv_weight[2] * padded[2:]

def reference(tokens, gate_pre, value_pre, up_gate_w, up_value_w, conv_weight, conv_bias, hidden_grad):
    col_count = FF // N_TP
    scale = float(TOKENS) ** (-0.5)

    def one_seq(carry, items):
        tok_rows, gate_rows, value_rows, grad_rows = items
        gate_float = gate_rows.astype(jnp.float32)
        gate_conv = conv_forward(gate_float, conv_weight, conv_bias)
        active, gelu_back = jax.vjp(jax.nn.gelu, gate_conv)
        grad_float = grad_rows.astype(jnp.float32)
        value_grad = (grad_float * active).astype(jnp.bfloat16)
        conv_grad = gelu_back(grad_float * value_rows.astype(jnp.float32))[0]
        shifted = jnp.pad(conv_grad, ((0, 2), (0, 0)))
        gate_grad = (conv_weight[2] * conv_grad + conv_weight[1] * shifted[1:ROWS + 1] + conv_weight[0] * shifted[2:]).astype(jnp.bfloat16)
        padded = jnp.pad(gate_float, ((2, 0), (0, 0)))
        conv_terms = jnp.stack([lax.optimization_barrier(jnp.sum(conv_grad * padded[:ROWS], axis=0)), lax.optimization_barrier(jnp.sum(conv_grad * padded[1:ROWS + 1], axis=0)), lax.optimization_barrier(jnp.sum(conv_grad * padded[2:], axis=0)), lax.optimization_barrier(jnp.sum(conv_grad, axis=0))])
        gate_term = jnp.dot(tok_rows.T, gate_grad, preferred_element_type=jnp.float32)
        value_term = jnp.dot(tok_rows.T, value_grad, preferred_element_type=jnp.float32)
        parts = jnp.einsum('rkc,dkc->krd', gate_grad.reshape(ROWS, N_TP, col_count).astype(jnp.float32), up_gate_w.reshape(D, N_TP, col_count).astype(jnp.float32))
        parts = parts + jnp.einsum('rkc,dkc->krd', value_grad.reshape(ROWS, N_TP, col_count).astype(jnp.float32), up_value_w.reshape(D, N_TP, col_count).astype(jnp.float32))
        rounded = lax.optimization_barrier(parts.astype(jnp.bfloat16))
        input_rows = lax.optimization_barrier(jnp.sum(rounded.astype(jnp.float32), axis=0)).astype(jnp.bfloat16)
        return ((carry[0] + gate_term, carry[1] + value_term, carry[2] + conv_terms), input_rows)
    init = (jnp.zeros((D, FF), jnp.float32), jnp.zeros((D, FF), jnp.float32), jnp.zeros((4, FF), jnp.float32))
    items = (tokens.reshape(N_FS, ROWS, D), gate_pre.reshape(N_FS, ROWS, FF), value_pre.reshape(N_FS, ROWS, FF), hidden_grad.reshape(N_FS, ROWS, FF))
    totals, input_seqs = lax.scan(one_seq, init, items)
    input_grad = input_seqs.reshape(TOKENS, D)
    conv_total = totals[2] * scale
    return (input_grad, totals[0] * scale, totals[1] * scale, conv_total[:3], conv_total[3])
```

```python
import jax
import jax.numpy as jnp
from jax import lax
from jax.sharding import PartitionSpec as P


def contract_rows(left, right):
    return lax.dot_general(
        left, right, (((0,), (0,)), ((), ())), preferred_element_type=jnp.float32
    )


def contract_cols(left, right):
    return lax.dot_general(
        left, right, (((1,), (1,)), ((), ())), preferred_element_type=jnp.float32
    )


def ring_of(count):
    return [*range(0, count, 2), *reversed(range(1, count, 2))]


def ring_gather(block, axis, backward, tie_step, tie):
    count = lax.axis_size(axis)
    ring = ring_of(count)
    if backward:
        ring = ring[::-1]
    hops = [(ring[i], ring[(i + 1) % count]) for i in range(count)]
    place = [ring.index(i) for i in range(count)]
    mine = jnp.asarray(place, jnp.int32)[lax.axis_index(axis)]
    order = jnp.asarray(ring, jnp.int32)
    rows = block.shape[0]
    whole = jnp.zeros((rows * count, block.shape[1]), block.dtype)
    for step in range(count):
        owner = order[(mine - step + count) % count]
        whole = lax.dynamic_update_slice(whole, block, (owner * rows, 0))
        if step < count - 1:
            if step == tie_step:
                block, tie = lax.optimization_barrier((block, tie))
            block = lax.ppermute(block, axis, hops)
    return whole


def sum_over(terms, axis):
    count = lax.axis_size(axis)
    if count & (count - 1):
        return lax.psum(terms, axis)
    reach = 1
    while reach < count:
        terms = terms + lax.ppermute(terms, axis, [(i, i ^ reach) for i in range(count)])
        reach *= 2
    return terms


def on_device(
    tokens, gate_pre, value_pre, up_gate_w, up_value_w, conv_weight, conv_bias, hidden_grad
):
    length = gate_pre.shape[0]
    col_count = gate_pre.shape[1]
    scale = float(length * lax.axis_size("fs")) ** (-0.5)
    gate_float = gate_pre.astype(jnp.float32)
    padded = jnp.pad(gate_float, ((2, 0), (0, 0)))
    gate_conv = (
        conv_bias
        + conv_weight[0] * padded[:length]
        + conv_weight[1] * padded[1 : length + 1]
        + conv_weight[2] * padded[2:]
    )
    active, gelu_back = jax.vjp(jax.nn.gelu, gate_conv)
    grad_float = hidden_grad.astype(jnp.float32)
    value_grad = (grad_float * active).astype(jnp.bfloat16)
    conv_grad = gelu_back(grad_float * value_pre.astype(jnp.float32))[0]
    shifted = jnp.pad(conv_grad, ((0, 2), (0, 0)))
    gate_grad = (
        conv_weight[2] * conv_grad
        + conv_weight[1] * shifted[1 : length + 1]
        + conv_weight[0] * shifted[2:]
    ).astype(jnp.bfloat16)
    conv_terms = jnp.stack(
        [
            jnp.sum(conv_grad * padded[:length], axis=0),
            jnp.sum(conv_grad * padded[1 : length + 1], axis=0),
            jnp.sum(conv_grad * padded[2:], axis=0),
            jnp.sum(conv_grad, axis=0),
        ]
    )
    conv_total = sum_over(conv_terms, "fs") * scale
    whole_tokens = lax.all_gather(tokens, "tp", axis=0, tiled=True)
    terms = [
        contract_rows(whole_tokens, grad).astype(jnp.bfloat16) for grad in (gate_grad, value_grad)
    ]
    full_gate = ring_gather(up_gate_w, "fs", False, 3, terms[0][:1, :1])
    full_value = ring_gather(up_value_w, "fs", True, 3, terms[0][:1, :1])
    gate_out, value_out = (
        lax.psum_scatter(
            term,
            "fs",
            scatter_dimension=0,
            tiled=True,
        ).astype(jnp.float32)
        * scale
        for term in terms
    )
    input_grad = lax.psum_scatter(
        (contract_cols(gate_grad, full_gate) + contract_cols(value_grad, full_value)).astype(
            jnp.bfloat16
        ),
        "tp",
        scatter_dimension=0,
        tiled=True,
    )
    return (input_grad, gate_out, value_out, conv_total[:3], conv_total[3])


def solution(mesh):
    return jax.shard_map(
        on_device,
        mesh=mesh,
        in_specs=(
            P(("fs", "tp"), None),
            P("fs", "tp"),
            P("fs", "tp"),
            P("fs", "tp"),
            P("fs", "tp"),
            P(None, "tp"),
            P("tp"),
            P("fs", "tp"),
        ),
        out_specs=(P(("fs", "tp"), None), P("fs", "tp"), P("fs", "tp"), P(None, "tp"), P("tp")),
        check_vma=False,
    )
```
